32 devices in a mesh: fs: 4 (over z), tp: 4 (over y, x), rep: 2 (over core).
Axes of the slice: x: 2, y: 2, z: 4, core: 2. Of those that a mesh axis runs over, the one named last changes fastest.
Arguments:
- gate_grads: float32 [2, 5632, 2048], P('rep', 'fs', 'tp'), may hold values from -16 to 16, as said below
- gate_velocity: float32 [5632, 2048], P(('fs', 'rep'), 'tp'), may hold values from -31 to 31, as said below
- gate_weight: float32 [5632, 2048], P(('fs', 'rep'), 'tp'), may hold values from -4 to 4
- up_grads: float32 [2, 5632, 2048], P('rep', 'fs', 'tp'), may hold values from -16 to 16, as said below
- up_velocity: float32 [5632, 2048], P(('fs', 'rep'), 'tp'), may hold values from -31 to 31, as said below
- up_weight: float32 [5632, 2048], P(('fs', 'rep'), 'tp'), may hold values from -4 to 4
- branch_grads: float32 [2, 2048, 1024], P('rep', 'fs', 'tp'), may hold values from -16 to 16, as said below
- branch_velocity: float32 [2048, 1024], P(('fs', 'rep'), 'tp'), may hold values from -31 to 31, as said below
- branch_weight: float32 [2048, 1024], P(('fs', 'rep'), 'tp'), may hold values from -4 to 4
Outputs:
- gate_momentum: float32 [5632, 2048], P(('fs', 'rep'), 'tp')
- gate_updated: float32 [5632, 2048], P(('fs', 'rep'), 'tp')
- up_momentum: float32 [5632, 2048], P(('fs', 'rep'), 'tp')
- up_updated: float32 [5632, 2048], P(('fs', 'rep'), 'tp')
- branch_momentum: float32 [2048, 1024], P(('fs', 'rep'), 'tp')
- branch_updated: float32 [2048, 1024], P(('fs', 'rep'), 'tp')
The draws below stay inside these ranges and needn't reach their ends.
Inputs may be any that keep to these rules, and one draw needn't show every extreme that they name: `gate_grads`: entries vary in scale over rows and over columns. `up_grads`: entries vary in scale over rows and over columns. `branch_grads`: entries vary in scale over rows and over columns. `gate_velocity`: entries vary in scale over rows and over columns. `up_velocity`: entries vary in scale over rows and over columns. `branch_velocity`: entries vary in scale over rows and over columns.
All inputs are finite; a program needn't handle non-finite values.
Results may differ from the reference program's by a relative error of at most 0.039.
Values may be sent and summed in bfloat16 or wider, within the bound.
A program may use at most 64 MiB of HBM per device.

```python
import math
import jax
import jax.numpy as jnp
from jax import lax

D = 2048
FF = 5632
BRANCH = 1024
ITERS = 3
REP = 2
N_FS = 4
N_REP = 2


def block_scaled(key, height, width):
    noise_key, row_key, col_key = jax.random.split(key, 3)
    noise = jnp.clip(jax.random.normal(noise_key, (height, width), jnp.float32), -4.0, 4.0)
    rise = math.log(4.0)
    row_factor = jnp.exp(jax.random.uniform(row_key, (8,), jnp.float32, -0.3, 0.3))
    col_factor = jnp.exp(jax.random.uniform(col_key, (4,), jnp.float32, -0.3, 0.3))
    row_ramp = jnp.exp(rise * (jnp.arange(height, dtype=jnp.float32) / (height - 1) - 1.0))
    col_ramp = jnp.exp(rise * (jnp.arange(width, dtype=jnp.float32) / (width - 1) - 1.0))
    row_scale = jnp.repeat(row_factor, height // 8) * row_ramp
    col_scale = jnp.repeat(col_factor, width // 4) * col_ramp
    return noise * row_scale[:, None] * col_scale[None, :]


def replicas(key, height, width):
    return jnp.stack([block_scaled(jax.random.fold_in(key, 11 + index), height, width) for index in range(REP)])


def draw_gate_grads(key, part):
    return replicas(key, FF, D)


def draw_up_grads(key, part):
    return replicas(jax.random.fold_in(key, 3), FF, D)


def draw_branch_grads(key, part):
    return replicas(jax.random.fold_in(key, 5), D, BRANCH)


def draw_gate_velocity(key, part):
    return 2.0 * block_scaled(jax.random.fold_in(key, 21), FF, D)


def draw_up_velocity(key, part):
    return 2.0 * block_scaled(jax.random.fold_in(key, 23), FF, D)


def draw_branch_velocity(key, part):
    return 2.0 * block_scaled(jax.random.fold_in(key, 25), D, BRANCH)


def steps_of(key, extent, cuts, smallest, high):
    def one(dim, parts):
        steps = jax.random.uniform(jax.random.fold_in(jax.random.fold_in(key, 6), dim), (parts,), jnp.float32, smallest / len(cuts), high / len(cuts))
        return jnp.repeat(jnp.exp(steps), extent[dim] // parts).reshape((-1,) + (1,) * (len(extent) - dim - 1))

    gain = one(*cuts[0])
    for cut in cuts[1:]:
        gain = gain * one(*cut)
    return gain


def normal_values(own_key, shape, scale, most, shards=(), kind=jnp.bfloat16):
    array = jax.random.normal(own_key, shape, jnp.float32) * scale
    if len(shards) > 0:
        array = steps_of(own_key, shape, shards, -0.22, 0.18) * array
    return jnp.clip(array, min=-most, max=most).astype(kind)


def setup_inputs(seed: int = 0) -> dict:
    keys = jax.random.split(jax.random.key(seed), 10)
    return {
        "gate_grads": draw_gate_grads(jax.random.fold_in(keys[9], 71), 0),
        "gate_velocity": draw_gate_velocity(jax.random.fold_in(keys[9], 71), 0),
        "gate_weight": normal_values(keys[2], (FF, D), 1.0, 4.0, ((0, 8), (1, 4)), jnp.float32),
        "up_grads": draw_up_grads(jax.random.fold_in(keys[9], 71), 0),
        "up_velocity": draw_up_velocity(jax.random.fold_in(keys[9], 71), 0),
        "up_weight": normal_values(keys[5], (FF, D), 1.0, 4.0, ((0, 8), (1, 4)), jnp.float32),
        "branch_grads": draw_branch_grads(jax.random.fold_in(keys[9], 71), 0),
        "branch_velocity": draw_branch_velocity(jax.random.fold_in(keys[9], 71), 0),
        "branch_weight": normal_values(keys[8], (D, BRANCH), 1.0, 4.0, ((0, 8), (1, 4)), jnp.float32),
    }


MOMENT = 0.95
COEF_ONE = 3.4445
COEF_THREE = -4.775
COEF_FIVE = 2.0315
SAFETY = 2.0
RATE = 0.5
SHRINK = 0.95

def block_gram(matrix):
    count = N_FS * N_REP
    height = matrix.shape[0] // count
    width = matrix.shape[1]
    stacked = matrix.reshape(count, height, width)

    def add_block(total, block):
        part = jnp.dot(block.T, block, preferred_element_type=jnp.float32)
        narrow = lax.optimization_barrier(part.astype(jnp.bfloat16))
        return (total + narrow.astype(jnp.float32), None)
    total, unused = lax.scan(add_block, jnp.zeros((width, width), jnp.float32), stacked)
    return total

def orthogonal(momentum):
    start = momentum.astype(jnp.bfloat16)
    first = jnp.sum(jnp.square(start.astype(jnp.float32)))
    raw = block_gram(start)
    second = jnp.sum(raw * raw)
    ratio = SAFETY * (second + 1.0) / (first + 1.0)
    scale = lax.rsqrt(ratio)
    gram = (raw / ratio).astype(jnp.bfloat16)
    ymat = (jnp.dot(start, gram, preferred_element_type=jnp.float32) * scale).astype(jnp.bfloat16)
    zmat = jnp.dot(ymat, gram, preferred_element_type=jnp.float32).astype(jnp.bfloat16)
    current = (COEF_ONE * scale * start.astype(jnp.float32) + COEF_THREE * ymat.astype(jnp.float32) + COEF_FIVE * zmat.astype(jnp.float32)).astype(jnp.bfloat16)
    for index in range(ITERS - 1):
        gram = block_gram(current).astype(jnp.bfloat16)
        ymat = jnp.dot(current, gram, preferred_element_type=jnp.float32).astype(jnp.bfloat16)
        zmat = jnp.dot(ymat, gram, preferred_element_type=jnp.float32).astype(jnp.bfloat16)
        current = (COEF_ONE * current.astype(jnp.float32) + COEF_THREE * ymat.astype(jnp.float32) + COEF_FIVE * zmat.astype(jnp.float32)).astype(jnp.bfloat16)
    return current

def one_matrix(grads, velocity, weight):
    momentum = MOMENT * velocity + lax.optimization_barrier(jnp.sum(grads, axis=0))
    final = orthogonal(momentum)
    updated = SHRINK * weight - RATE * math.sqrt(weight.shape[0]) * final.astype(jnp.float32)
    return (momentum, updated)

def reference(gate_grads, gate_velocity, gate_weight, up_grads, up_velocity, up_weight, branch_grads, branch_velocity, branch_weight):
    gate_momentum, gate_updated = one_matrix(gate_grads, gate_velocity, gate_weight)
    up_momentum, up_updated = one_matrix(up_grads, up_velocity, up_weight)
    branch_momentum, branch_updated = one_matrix(branch_grads, branch_velocity, branch_weight)
    return (gate_momentum, gate_updated, up_momentum, up_updated, branch_momentum, branch_updated)
```

```python
import functools
import math

import jax
import jax.numpy as jnp
from jax import lax
from jax.experimental import pallas as pl
from jax.experimental.pallas import tpu as pltpu
from jax.sharding import PartitionSpec as P

MOMENT = 0.95
COEF_ONE = 3.4445
COEF_THREE = -4.775
COEF_FIVE = 2.0315
SAFETY = 2.0
RATE = 0.5
SHRINK = 0.95
ITERS = 3
TILE = 512


def polynomial_kernel(size, tile, scale_ref, g_ref, q_ref, s0, s1, s2, s3):
    count = size // tile
    pairs = count * (count + 1) // 2

    def product(left, right, out, finish):
        def step(t, carry):
            i = lax.rem(t, count)
            j = lax.rem(i + t // count, count)
            rows = pl.ds(pl.multiple_of(i * tile, tile), tile)
            cols = pl.ds(pl.multiple_of(j * tile, tile), tile)
            acc = jnp.dot(left[rows, :], right[:, cols], preferred_element_type=jnp.float32)
            value = finish(acc, rows, cols, i == j).astype(jnp.bfloat16)
            out[rows, cols] = value

            @pl.when(i != j)
            def _():
                out[cols, rows] = value.T

            return carry

        lax.fori_loop(0, pairs, step, 0)

    def plain(acc, rows, cols, diagonal):
        return acc

    def scaled(acc, rows, cols, diagonal):
        return acc * scale_ref[0, 0]

    def quadratic(gram):
        def finish(acc, rows, cols, diagonal):
            here = lax.broadcasted_iota(jnp.int32, (tile, tile), 0)
            there = lax.broadcasted_iota(jnp.int32, (tile, tile), 1)
            unit = jnp.where(diagonal, COEF_ONE, 0.0)
            eye = jnp.where(here == there, unit, 0.0)
            return eye + COEF_THREE * gram[rows, cols].astype(jnp.float32) + COEF_FIVE * acc

        return finish

    product(g_ref, g_ref, s0, quadratic(g_ref))
    product(g_ref, s0, s1, plain)
    product(s1, s0, s2, plain)
    product(s2, s2, s1, quadratic(s2))
    product(s0, s1, s3, plain)
    product(s2, s1, s0, plain)
    product(s0, s1, q_ref, plain)
    product(q_ref, q_ref, s0, quadratic(q_ref))
    product(s3, s0, q_ref, scaled)


def polynomial(gram, scale):
    size = gram.shape[0]
    tile = min(TILE, size)
    matrix = pltpu.VMEM((size, size), jnp.bfloat16)
    return pl.pallas_call(
        functools.partial(polynomial_kernel, size, tile),
        out_shape=jax.ShapeDtypeStruct((size, size), jnp.bfloat16),
        in_specs=[
            pl.BlockSpec(memory_space=pltpu.SMEM),
            pl.BlockSpec(memory_space=pltpu.VMEM),
        ],
        out_specs=pl.BlockSpec(memory_space=pltpu.VMEM),
        scratch_shapes=[matrix] * 4,
        compiler_params=pltpu.CompilerParams(
            vmem_limit_bytes=min(64000 * 1024, 6 * 2 * size * size + 12 * 1024 * 1024)
        ),
        cost_estimate=pl.CostEstimate(
            flops=12 * size**3, bytes_accessed=4 * size * size, transcendentals=0
        ),
        name=f"polynomial_{size}",
    )(scale.reshape(1, 1), gram)


def normalized(raw):
    wide = raw.astype(jnp.float32)
    size = raw.shape[0]
    here = lax.broadcasted_iota(jnp.int32, (size, size), 0)
    there = lax.broadcasted_iota(jnp.int32, (size, size), 1)
    first = jnp.sum(jnp.where(here == there, wide, 0.0))
    second = jnp.sum(wide * wide)
    ratio = SAFETY * (second + 1.0) / (first + 1.0)
    return (wide / ratio).astype(jnp.bfloat16), lax.rsqrt(ratio)


def partial_gram(whole, current):
    return lax.dot_general(
        whole, current, (((0,), (0,)), ((), ())), preferred_element_type=jnp.float32
    ).astype(jnp.bfloat16)


def assemble(blocks, down, across):
    _, height, width = blocks.shape
    grid = blocks.reshape(down, across, height, width).transpose(0, 2, 1, 3)
    return grid.reshape(down * height, across * width)


def local(nfs, ntp, nrep, *args):
    grads, velocities, weights = args[0::3], args[1::3], args[2::3]
    totals = [
        lax.psum_scatter(g.astype(jnp.bfloat16), "rep", scatter_dimension=1, tiled=True)[0]
        for g in grads
    ]
    moments = [MOMENT * v + t.astype(jnp.float32) for v, t in zip(velocities, totals)]
    starts = [moment.astype(jnp.bfloat16) for moment in moments]
    wholes = [lax.all_gather(start, "tp", axis=1, tiled=True) for start in starts]
    parts = [partial_gram(whole, start) for whole, start in zip(wholes, starts)]

    size, width = parts[0].shape
    pair = jnp.stack([part.reshape(nfs, size // nfs, width) for part in parts[:nrep]], axis=1)
    share = lax.psum_scatter(
        pair.reshape(nrep * size, width), ("fs", "rep"), scatter_dimension=0, tiled=True
    )
    blocks = lax.all_gather(share, ("fs", "tp"), axis=0, tiled=False)
    gram, scale = normalized(assemble(blocks, nfs, ntp))
    large = polynomial(gram, scale)
    column = lax.axis_index("tp") * width
    mine = lax.dynamic_slice(large, (0, column), (size, width))
    columns = lax.all_gather(mine, "rep", axis=0, tiled=False)

    last = lax.psum_scatter(parts[nrep], ("fs", "rep"), scatter_dimension=0, tiled=True)
    blocks = lax.all_gather(last, ("fs", "rep", "tp"), axis=0, tiled=False)
    gram, scale = normalized(assemble(blocks, nfs * nrep, ntp))
    small = polynomial(gram, scale)
    height, width = parts[nrep].shape
    column = lax.axis_index("tp") * width
    factors = [columns[index] for index in range(nrep)]
    factors.append(lax.dynamic_slice(small, (0, column), (height, width)))

    results = []
    for moment, weight, whole, factor in zip(moments, weights, wholes, factors):
        rows = moment.shape[0] * nfs * nrep
        final = jnp.dot(whole, factor, preferred_element_type=jnp.float32)
        results.append(moment)
        results.append(SHRINK * weight - RATE * math.sqrt(rows) * final)
    return tuple(results)


def solution(mesh):
    sizes = mesh.shape
    split = P(("fs", "rep"), "tp")
    return jax.shard_map(
        functools.partial(local, sizes["fs"], sizes["tp"], sizes["rep"]),
        mesh=mesh,
        in_specs=(P("rep", "fs", "tp"), split, split) * 3,
        out_specs=(split,) * 6,
        check_vma=False,
    )
```

```python
import functools
import math

import jax
import jax.numpy as jnp
from jax import lax
from jax.experimental import pallas as pl
from jax.experimental.pallas import tpu as pltpu
from jax.sharding import PartitionSpec as P

MOMENT = 0.95
COEF_ONE = 3.4445
COEF_THREE = -4.775
COEF_FIVE = 2.0315
SAFETY = 2.0
RATE = 0.5
SHRINK = 0.95
ITERS = 3
TILE = 512


def polynomial_kernel(across, tile, column_ref, raw_ref, q_ref, g, s0, s1, s2, s3, c0, c1):
    blocks, height, breadth = raw_ref.shape
    size, width = q_ref.shape
    count = size // tile
    pairs = count * (count + 1) // 2
    here = lax.broadcasted_iota(jnp.int32, (height, breadth), 0)
    there = lax.broadcasted_iota(jnp.int32, (height, breadth), 1)

    def sums(t, carry):
        first, second = carry
        wide = raw_ref[t].astype(jnp.float32)
        shift = lax.rem(t, across) * breadth - t // across * height
        trace = jnp.where(here == there + shift, wide, 0.0)
        return (
            first + jnp.sum(trace, axis=0, keepdims=True),
            second + jnp.sum(wide * wide, axis=0, keepdims=True),
        )

    zero = jnp.zeros((1, breadth), jnp.float32)
    first, second = lax.fori_loop(0, blocks, sums, (zero, zero))
    first = jnp.sum(first, axis=1, keepdims=True)
    second = jnp.sum(second, axis=1, keepdims=True)
    ratio = SAFETY * (second + 1.0) / (first + 1.0)
    inverse, scale = 1.0 / ratio, lax.rsqrt(ratio)

    def normalize(t, carry):
        rows = pl.ds(pl.multiple_of(t // across * height, height), height)
        cols = pl.ds(pl.multiple_of(lax.rem(t, across) * breadth, breadth), breadth)
        g[rows, cols] = (raw_ref[t].astype(jnp.float32) * inverse).astype(jnp.bfloat16)
        return carry

    lax.fori_loop(0, blocks, normalize, 0)

    def quadratic(acc, gram, shift):
        down = lax.broadcasted_iota(jnp.int32, acc.shape, 0)
        over = lax.broadcasted_iota(jnp.int32, acc.shape, 1)
        eye = jnp.where(down == over + shift, COEF_ONE, 0.0)
        return eye + COEF_THREE * gram.astype(jnp.float32) + COEF_FIVE * acc

    def product(left, right, out, poly):
        def step(t, carry):
            i = lax.rem(t, count)
            j = lax.rem(i + t // count, count)
            rows = pl.ds(pl.multiple_of(i * tile, tile), tile)
            cols = pl.ds(pl.multiple_of(j * tile, tile), tile)
            acc = jnp.dot(left[rows, :], right[:, cols], preferred_element_type=jnp.float32)
            if poly:
                acc = quadratic(acc, left[rows, cols], (j - i) * tile)
            value = acc.astype(jnp.bfloat16)
            out[rows, cols] = value

            @pl.when(i != j)
            def _():
                out[cols, rows] = value.T

            return carry

        lax.fori_loop(0, pairs, step, 0)

    column = pl.multiple_of(column_ref[0, 0] * width, width)
    mine = pl.ds(column, width)

    def panel(left, right, out, kind):
        def step(i, carry):
            rows = pl.ds(pl.multiple_of(i * tile, tile), tile)
            acc = jnp.dot(left[rows, :], right[...], preferred_element_type=jnp.float32)
            if kind == "poly":
                acc = quadratic(acc, left[rows, mine], column - i * tile)
            if kind == "scale":
                acc = acc * scale
            out[rows, :] = acc.astype(jnp.bfloat16)
            return carry

        lax.fori_loop(0, count, step, 0)

    product(g, g, s0, True)
    product(g, s0, s1, False)
    product(s1, s0, s2, False)
    product(s2, s2, s1, True)
    product(s2, s1, s3, False)
    product(s3, s1, g, False)
    c1[...] = g[:, mine]
    panel(g, c1, c0, "poly")
    panel(s1, c0, c1, "")
    panel(s0, c1, q_ref, "scale")


def polynomial(blocks, across):
    size = blocks.shape[2] * across
    width = blocks.shape[2]
    tile = min(TILE, size)
    matrix = pltpu.VMEM((size, size), jnp.bfloat16)
    strip = pltpu.VMEM((size, width), jnp.bfloat16)
    return pl.pallas_call(
        functools.partial(polynomial_kernel, across, tile),
        out_shape=jax.ShapeDtypeStruct((size, width), jnp.bfloat16),
        in_specs=[
            pl.BlockSpec(memory_space=pltpu.SMEM),
            pl.BlockSpec(memory_space=pltpu.VMEM),
        ],
        out_specs=pl.BlockSpec(memory_space=pltpu.VMEM),
        scratch_shapes=[matrix] * 5 + [strip] * 2,
        compiler_params=pltpu.CompilerParams(
            vmem_limit_bytes=12 * size * size + 6 * size * width + 8 * 1024 * 1024
        ),
        cost_estimate=pl.CostEstimate(
            flops=10 * size**3, bytes_accessed=3 * size * size, transcendentals=0
        ),
        name=f"polynomial_{size}",
    )(lax.axis_index("tp").astype(jnp.int32).reshape(1, 1), blocks)


def partial_gram(whole, current):
    return lax.dot_general(
        whole, current, (((0,), (0,)), ((), ())), preferred_element_type=jnp.float32
    ).astype(jnp.bfloat16)


def local(nfs, ntp, nrep, *args):
    grads, velocities, weights = args[0::3], args[1::3], args[2::3]
    totals = [
        lax.psum_scatter(g.astype(jnp.bfloat16), "rep", scatter_dimension=1, tiled=True)[0]
        for g in grads
    ]
    moments = [MOMENT * v + t.astype(jnp.float32) for v, t in zip(velocities, totals)]
    starts = [moment.astype(jnp.bfloat16) for moment in moments]
    starts = lax.optimization_barrier(starts)
    wholes = [lax.all_gather(start, "tp", axis=1, tiled=True) for start in starts]
    parts = [partial_gram(whole, start) for whole, start in zip(wholes, starts)]

    shares = nfs * nrep
    size, width = parts[0].shape
    depth, narrow = parts[nrep].shape
    fold = width // narrow
    pair = jnp.stack([part.reshape(nfs, size // nfs, width) for part in parts[:nrep]], axis=1)
    pair = pair.reshape(shares, size // nfs, width)
    third = parts[nrep].reshape(shares, fold, depth // shares // fold, narrow)
    third = jnp.concatenate([third[:, index] for index in range(fold)], axis=2)
    both = jnp.concatenate([pair, third], axis=1)
    share = lax.psum_scatter(
        both.reshape(-1, width), ("fs", "rep"), scatter_dimension=0, tiled=True
    )
    blocks = lax.all_gather(share[: size // nfs], ("fs", "tp"), axis=0, tiled=False)
    tail = share[size // nfs :]
    last = jnp.concatenate(
        [tail[:, index * narrow : (index + 1) * narrow] for index in range(fold)], axis=0
    )
    blocks, last = lax.optimization_barrier((blocks, last))
    gathered = lax.all_gather(last, ("fs", "rep", "tp"), axis=0, tiled=False)
    mine = polynomial(blocks, ntp)
    columns = lax.all_gather(mine, "rep", axis=0, tiled=False)
    factors = [columns[index] for index in range(nrep)]
    factors.append(polynomial(gathered, ntp))

    results = []
    for moment, weight, whole, factor in zip(moments, weights, wholes, factors):
        rows = moment.shape[0] * nfs * nrep
        final = jnp.dot(whole, factor, preferred_element_type=jnp.float32)
        results.append(moment)
        results.append(SHRINK * weight - RATE * math.sqrt(rows) * final)
    return tuple(results)


def solution(mesh):
    sizes = mesh.shape
    split = P(("fs", "rep"), "tp")
    return jax.shard_map(
        functools.partial(local, sizes["fs"], sizes["tp"], sizes["rep"]),
        mesh=mesh,
        in_specs=(P("rep", "fs", "tp"), split, split) * 3,
        out_specs=(split,) * 6,
        check_vma=False,
    )
```
